32 devices in a mesh: fs: 16 (over z, y, x), tp: 2 (over core).
Axes of the slice: x: 2, y: 2, z: 4, core: 2. Of those that a mesh axis runs over, the one named last changes fastest.
Arguments:
- saved_inputs: bfloat16 [12288, 2048], P('fs'), may hold values from -8 to 8
- input_cot: bfloat16 [12288, 2048], P('fs', 'tp'), may hold values from -0.0546875 to 0.0546875
- gate_cot: bfloat16 [12288, 2048], P('fs', 'tp'), may hold values from -0.0546875 to 0.0546875
- input_master: float32 [2048, 2048], P('fs', 'tp'), may hold values from -6 to 6
- gate_master: float32 [2048, 2048], P('fs', 'tp'), may hold values from -6 to 6
- input_factor: bfloat16 [2048, 256], P('fs'), may hold values from -2 to 2
- gate_factor: bfloat16 [2048, 256], P('fs'), may hold values from -2 to 2
- input_first: float32 [256, 2048], P('fs', 'tp'), may hold values from -6 to 6
- input_second: float32 [256, 2048], P('fs', 'tp'), may hold values from 0.2 to 17
- gate_first: float32 [256, 2048], P('fs', 'tp'), may hold values from -6 to 6
- gate_second: float32 [256, 2048], P('fs', 'tp'), may hold values from 0.2 to 17
Outputs:
- input_step: float32 [2048, 2048], P('fs', 'tp')
- gate_step: float32 [2048, 2048], P('fs', 'tp')
- input_first_new: float32 [256, 2048], P('fs', 'tp')
- input_second_new: float32 [256, 2048], P('fs', 'tp')
- gate_first_new: float32 [256, 2048], P('fs', 'tp')
- gate_second_new: float32 [256, 2048], P('fs', 'tp')
- input_copy: bfloat16 [2048, 2048], P(None, 'tp')
- gate_copy: bfloat16 [2048, 2048], P(None, 'tp')
The draws below stay inside these ranges and needn't reach their ends.
All inputs are finite; a program needn't handle non-finite values.
Results may differ from the reference program's by a relative error of at most 0.0004.
Values may be sent and summed in bfloat16 or wider, within the bound.
No kernel may reach another device: no remote copies, remote signals or barrier semaphores. Data moves between devices by JAX's collectives and lax.ppermute only.
A program may use at most 64 MiB of HBM per device.

```python
import jax
import jax.numpy as jnp
from jax import lax

D = 2048
W = 2048
RANK = 256
TOKENS = 12288


def factor_draw(key, salt):
    keyed = jax.random.fold_in(key, salt)
    key_one, key_two = jax.random.split(keyed)
    position = jnp.arange(D, dtype=jnp.float32)[:, None] / D
    jitter = jnp.exp(jax.random.uniform(key_one, (D, 1), jnp.float32, -0.7, 0.7))
    scales = jnp.exp(jnp.log(6.0) * position) * jitter / 2.8
    entries = jax.random.normal(key_two, (D, RANK), jnp.float32)
    values = jnp.clip(entries * scales * D ** (-0.5), -2.0, 2.0)
    return values.astype(jnp.bfloat16)


def second_draw(key, salt):
    keyed = jax.random.fold_in(key, salt)
    column = jnp.arange(W, dtype=jnp.float32)[None, :] / W
    jitter = jnp.exp(jax.random.uniform(keyed, (RANK, W), jnp.float32, -0.7, 0.7))
    spread = jnp.exp(jnp.log(9.0) * (1.0 - column))
    return (0.5 * jitter * spread).astype(jnp.float32)


def draw_input_factor(key, part):
    return factor_draw(key, 11)


def draw_gate_factor(key, part):
    return factor_draw(key, 23)


def draw_input_second(key, part):
    return second_draw(key, 37)


def draw_gate_second(key, part):
    return second_draw(key, 41)


def raised(result, key, source, target, shards_of, factor):
    owner, partner = [(jnp.arange(result.shape[axis_at]) // (result.shape[axis_at] // shards_of)).reshape([-1 if axis == axis_at else 1 for axis in range(result.ndim)]) for axis_at in (source, target)]
    chosen = jax.random.permutation(key, shards_of)[partner]
    strong = (owner == chosen) | (owner == (partner + shards_of // 2) % shards_of)
    return jnp.where(strong, factor * result, result)


def block_levels(own_key, shape, shards, smallest, high):
    loudness = 1.0
    for axis_at, parts in shards:
        heights = jax.random.uniform(jax.random.fold_in(jax.random.fold_in(own_key, 6), axis_at), (parts,), jnp.float32, smallest / len(shards), high / len(shards))
        loudness = loudness * jnp.repeat(jnp.exp(heights), shape[axis_at] // parts).reshape((-1,) + (1,) * (len(shape) - 1 - axis_at))
    return loudness


def gaussian(own_key, shape, scale, most, cuts=(), kind=jnp.bfloat16):
    values = scale * jax.random.normal(own_key, shape, jnp.float32)
    if cuts:
        values = values * block_levels(own_key, shape, cuts, -0.22, 0.18)
    return jnp.clip(values, -most, most).astype(kind)


def gaussian_with(own_key, dims, deviation, reach, shards, heavy, kind=jnp.bfloat16):
    values = deviation * jax.random.normal(own_key, dims, jnp.float32)
    if shards:
        values = values * block_levels(own_key, dims, shards, -0.22, 0.18)
    return jnp.clip(raised(values, jax.random.fold_in(own_key, 3), *heavy), -reach, reach).astype(kind)


def setup_inputs(seed: int = 0) -> dict:
    key_of = jax.random.split(jax.random.key(seed), 12)
    saved_inputs = gaussian_with(key_of[0], (TOKENS, D), 1.0, 8.0, ((0, 16),), (0, 1, 16, 2.0))
    input_cot = gaussian(key_of[1], (TOKENS, W), (TOKENS ** -0.5), 0.0546875, ((0, 16), (1, 2)))
    gate_cot = gaussian(key_of[2], (TOKENS, W), (TOKENS ** -0.5), 0.0546875, ((0, 16), (1, 2)))
    input_master = gaussian(key_of[3], (D, W), 1.0, 6.0, ((0, 16), (1, 2)), jnp.float32)
    gate_master = gaussian(key_of[4], (D, W), 1.0, 6.0, ((0, 16), (1, 2)), jnp.float32)
    input_factor = draw_input_factor(jax.random.fold_in(key_of[11], 71), 0)
    gate_factor = draw_gate_factor(jax.random.fold_in(key_of[11], 71), 0)
    input_first = gaussian(key_of[7], (RANK, W), 1.0, 6.0, ((0, 16), (1, 2)), jnp.float32)
    input_second = draw_input_second(jax.random.fold_in(key_of[11], 71), 0)
    gate_first = gaussian(key_of[9], (RANK, W), 1.0, 6.0, ((0, 16), (1, 2)), jnp.float32)
    gate_second = draw_gate_second(jax.random.fold_in(key_of[11], 71), 0)
    return {"saved_inputs": saved_inputs, "input_cot": input_cot, "gate_cot": gate_cot, "input_master": input_master, "gate_master": gate_master, "input_factor": input_factor, "gate_factor": gate_factor, "input_first": input_first, "input_second": input_second, "gate_first": gate_first, "gate_second": gate_second}


first_decay = 0.9
second_decay = 0.9
ratio_floor = 1e-08
mean_floor = 1e-06
step_size = 0.05

def update_one(saved_inputs, cotangent, master, factor, first, second):
    contract = (((0,), (0,)), ((), ()))
    gradient = lax.dot_general(saved_inputs, cotangent, contract, preferred_element_type=jnp.float32)
    factor_wide = factor.astype(jnp.float32)
    low_rank = lax.dot_general(factor_wide, gradient, contract, precision=lax.Precision.HIGHEST)
    first_new = first_decay * first + (1.0 - first_decay) * low_rank
    second_new = second_decay * second + (1.0 - second_decay) * low_rank * low_rank
    ratio = first_new / (jnp.sqrt(second_new) + ratio_floor)
    direction = jnp.dot(factor_wide, ratio, precision=lax.Precision.HIGHEST)
    step = direction * lax.rsqrt(jnp.mean(direction * direction) + mean_floor)
    weights_copy = (master - step_size * step).astype(jnp.bfloat16)
    return (step, first_new, second_new, weights_copy)

def reference(saved_inputs, input_cot, gate_cot, input_master, gate_master, input_factor, gate_factor, input_first, input_second, gate_first, gate_second):
    step_in, first_in, second_in, copy_in = update_one(saved_inputs, input_cot, input_master, input_factor, input_first, input_second)
    step_gate, first_gate, second_gate, copy_gate = update_one(saved_inputs, gate_cot, gate_master, gate_factor, gate_first, gate_second)
    return (step_in, step_gate, first_in, second_in, first_gate, second_gate, copy_in, copy_gate)
```

```python
import jax
import jax.numpy as jnp
from jax import lax
from jax.experimental import pallas as pl
from jax.experimental.pallas import tpu as pltpu
from jax.sharding import PartitionSpec as P

first_decay = 0.9
second_decay = 0.9
ratio_floor = 1e-08
mean_floor = 1e-06
step_size = 0.05
bf16 = jnp.bfloat16
f32 = jnp.float32
contract = (((0,), (0,)), ((), ()))
plain = (((1,), (0,)), ((), ()))


def swap(a, axis, mask):
    size = lax.axis_size(axis)
    return lax.ppermute(a, axis, [(i, i ^ mask) for i in range(size)])


def split(a, terms):
    out = []
    for _ in range(terms):
        top = lax.reduce_precision(a, 8, 7)
        out.append(top.astype(bf16))
        a = a - top
    return out


def dot(a, b, dims):
    return lax.dot_general(a, b, dims, preferred_element_type=f32)


def moments(low_rank, first, second):
    first_new = first_decay * first + (1.0 - first_decay) * low_rank
    second_new = second_decay * second + (1.0 - second_decay) * low_rank * low_rank
    ratio = first_new / (jnp.sqrt(second_new) + ratio_floor)
    return (first_new, second_new, ratio)


def pick(a, index, axis):
    return lax.dynamic_index_in_dim(a, index, axis, keepdims=False)


def gather(own, halves):
    cut, join = halves
    lines = lax.axis_size("fs") // 4
    blocks = {0: own}
    for k in range(1, lines):
        blocks[4 * k] = swap(own, "fs", 4 * k)
    blocks[1] = swap(own, "fs", 1)
    blocks[2] = swap(own, "fs", 2)
    if lines > 1:
        stack = jnp.stack([blocks[4 * k] for k in range(1, lines)])
        across = swap(stack, "fs", 1)
        along = swap(stack, "fs", 2)
        for k in range(1, lines):
            blocks[4 * k + 1] = across[k - 1]
            blocks[4 * k + 2] = along[k - 1]
    one = swap(jnp.stack([cut(blocks[4 * k + 1])[0] for k in range(lines)]), "fs", 2)
    two = swap(jnp.stack([cut(blocks[4 * k + 2])[1] for k in range(lines)]), "fs", 1)
    for k in range(lines):
        blocks[4 * k + 3] = join(one[k], two[k])
    return blocks


def place(blocks, me):
    rows, columns = blocks[0].shape
    whole = jnp.zeros((len(blocks), rows, columns), blocks[0].dtype)
    for mask, block in blocks.items():
        whole = lax.dynamic_update_index_in_dim(whole, block, me ^ mask, 0)
    return whole.reshape(len(blocks) * rows, columns)


def spread(own):
    blocks = {}
    for k in range(lax.axis_size("fs") // 4):
        block = swap(own, "fs", 4 * k) if k else own
        across = swap(block, "fs", 1)
        along = swap(block, "fs", 2)
        corner = swap(along, "fs", 1) if k % 2 else swap(across, "fs", 2)
        blocks |= {4 * k: block, 4 * k + 1: across, 4 * k + 2: along, 4 * k + 3: corner}
    return blocks


def write_copies(blocks, factor, ratio, scale, me):
    count = len(blocks)
    rows, width = blocks[0].shape
    rank = ratio.shape[0]
    order = list(blocks)

    def kernel(me_ref, scale_ref, factor_ref, ratio_ref, *rest):
        masters, (out, terms, held, ready, load, store) = rest[:count], rest[count:]

        def fetch(i):
            return pltpu.make_async_copy(masters[i], held.at[i % 3], load.at[i % 3])

        def flush(i):
            owner = me_ref[0] ^ order[i]
            target = out.at[pl.ds(pl.multiple_of(owner * rows, rows), rows), :]
            return pltpu.make_async_copy(ready.at[i % 2], target, store.at[i % 2])

        fetch(0).start()
        fetch(1).start()
        rest_of = ratio_ref[...]
        for i in range(3):
            top = rest_of.astype(bf16)
            terms[i * rank : (i + 1) * rank, :] = top
            rest_of = rest_of - top.astype(f32)
        shrink = step_size * scale_ref[0]
        for i in range(count):
            if i + 2 < count:
                fetch(i + 2).start()
            owner = me_ref[0] ^ order[i]
            some = factor_ref[pl.ds(pl.multiple_of(owner * rows, rows), rows), :]
            moved = jnp.dot(
                jnp.concatenate([some] * 3, axis=1), terms[...], preferred_element_type=f32
            )
            fetch(i).wait()
            if i >= 2:
                flush(i - 2).wait()
            ready[i % 2] = (held[i % 3] - shrink * moved).astype(bf16)
            flush(i).start()
        for i in range(max(count - 2, 0), count):
            flush(i).wait()

    smem, vmem, anywhere = (
        pl.BlockSpec(memory_space=space) for space in (pltpu.SMEM, pltpu.VMEM, pl.ANY)
    )
    return pl.pallas_call(
        kernel,
        out_shape=jax.ShapeDtypeStruct((count * rows, width), bf16),
        in_specs=[smem, smem, vmem, vmem] + [anywhere] * count,
        out_specs=anywhere,
        scratch_shapes=[
            pltpu.VMEM((3 * rank, width), bf16),
            pltpu.VMEM((3, rows, width), f32),
            pltpu.VMEM((2, rows, width), bf16),
            pltpu.SemaphoreType.DMA((3,)),
            pltpu.SemaphoreType.DMA((2,)),
        ],
        compiler_params=pltpu.CompilerParams(vmem_limit_bytes=16 * 2**20),
        cost_estimate=pl.CostEstimate(
            flops=6 * count * rows * rank * width, bytes_accessed=6 * count * rows * width, transcendentals=0
        ),
        name="write_copies",
    )(me.astype(jnp.int32).reshape(1), scale.reshape(1), factor, ratio, *blocks.values())


def local(
    saved_inputs,
    input_cot,
    gate_cot,
    input_master,
    gate_master,
    input_factor,
    gate_factor,
    input_first,
    input_second,
    gate_first,
    gate_second,
):
    fs, tp = lax.axis_size("fs"), lax.axis_size("tp")
    me, core = lax.axis_index("fs"), lax.axis_index("tp")
    lines = fs // 4
    here_x, here_y, here_z = me & 1, (me >> 1) & 1, me >> 2
    rank = input_factor.shape[1]
    width = input_cot.shape[1]
    rank_rows = rank // fs

    by_rows = (
        lambda a: (a[: a.shape[0] // 2], a[a.shape[0] // 2 :]),
        lambda a, b: jnp.concatenate([a, b]),
    )
    masters = spread(input_master)
    if tp == 2:
        whole = place(gather(jnp.where(core == 0, input_factor, gate_factor), by_rows), me)
        other = swap(whole, "tp", 1)
        whole_in = jnp.where(core == 0, whole, other)
        whole_gate = jnp.where(core == 0, other, whole)
    else:
        whole_in = place(gather(input_factor, by_rows), me)
        whole_gate = place(gather(gate_factor, by_rows), me)

    def low_term(factor, cot):
        projected = dot(saved_inputs, factor, plain)
        return sum(dot(piece, cot, contract) for piece in split(projected, 2))

    term_in = low_term(whole_in, input_cot).reshape(lines, 2, 2, rank_rows, width)
    term_gate = low_term(whole_gate, gate_cot).reshape(lines, 2, 2, rank_rows, width)
    gram_in = dot(whole_in, whole_in, contract)
    gram_gate = dot(whole_gate, whole_gate, contract)

    part_in = pick(term_in, here_x, 2) + swap(pick(term_in, 1 - here_x, 2), "fs", 1)
    part_gate = pick(term_gate, here_y, 1) + swap(pick(term_gate, 1 - here_y, 1), "fs", 2)
    part_in = pick(part_in, here_y, 1) + swap(pick(part_in, 1 - here_y, 1), "fs", 2)
    part_gate = pick(part_gate, here_x, 1) + swap(pick(part_gate, 1 - here_x, 1), "fs", 1)
    both = jnp.stack([part_in, part_gate], axis=1)
    summed = pick(both, here_z, 0)
    for k in range(1, lines):
        summed = summed + swap(pick(both, here_z ^ k, 0), "fs", 4 * k)

    first_in, second_in, ratio_in = moments(summed[0], input_first, input_second)
    first_gate, second_gate, ratio_gate = moments(summed[1], gate_first, gate_second)
    by_kind = (lambda a: (a[:1], a[1:]), lambda a, b: jnp.concatenate([a, b]))
    ratios = gather(jnp.stack([ratio_in, ratio_gate]), by_kind)
    piece_in = place({mask: block[0] for mask, block in ratios.items()}, me)
    piece_gate = place({mask: block[1] for mask, block in ratios.items()}, me)

    def square(gram, ratio):
        return jnp.sum(ratio * jnp.dot(gram, ratio, precision=lax.Precision.HIGHEST))

    def direction(factor, ratio):
        return sum(dot(factor, piece, plain) for piece in split(ratio, 3))

    def total(square):
        return square + swap(square, "tp", 1) if tp == 2 else lax.psum(square, "tp")

    count = fs * input_master.shape[0] * tp * width
    scale_gate = lax.rsqrt(total(square(gram_gate, piece_gate)) / count + mean_floor)
    scale_in = lax.rsqrt(total(square(gram_in, piece_in)) / count + mean_floor)
    step_gate = direction(gate_factor, piece_gate) * scale_gate
    step_in = direction(input_factor, piece_in) * scale_in
    copy_gate = place(spread((gate_master - step_size * step_gate).astype(bf16)), me)
    copy_in = write_copies(masters, whole_in, piece_in, scale_in, me)
    return (step_in, step_gate, first_in, second_in, first_gate, second_gate, copy_in, copy_gate)


def solution(mesh):
    rows, tokens = P("fs", "tp"), P("fs", None)
    return jax.shard_map(
        local,
        mesh=mesh,
        in_specs=(tokens, rows, rows, rows, rows, tokens, tokens, rows, rows, rows, rows),
        out_specs=(rows,) * 6 + (P(None, "tp"),) * 2,
        check_vma=False,
    )
```

```python
import jax
import jax.numpy as jnp
from jax import lax
from jax.experimental import pallas as pl
from jax.experimental.pallas import tpu as pltpu
from jax.sharding import PartitionSpec as P

first_decay = 0.9
second_decay = 0.9
ratio_floor = 1e-08
mean_floor = 1e-06
step_size = 0.05
bf16 = jnp.bfloat16
f32 = jnp.float32
contract = (((0,), (0,)), ((), ()))
plain = (((1,), (0,)), ((), ()))


def swap(a, axis, mask):
    size = lax.axis_size(axis)
    return lax.ppermute(a, axis, [(i, i ^ mask) for i in range(size)])


def split(a, terms):
    out = []
    for _ in range(terms):
        top = lax.reduce_precision(a, 8, 7)
        out.append(top.astype(bf16))
        a = a - top
    return out


def dot(a, b, dims):
    return lax.dot_general(a, b, dims, preferred_element_type=f32)


def moments(low_rank, first, second):
    first_new = first_decay * first + (1.0 - first_decay) * low_rank
    second_new = second_decay * second + (1.0 - second_decay) * low_rank * low_rank
    ratio = first_new / (jnp.sqrt(second_new) + ratio_floor)
    return (first_new, second_new, ratio)


def pick(a, index, axis):
    return lax.dynamic_index_in_dim(a, index, axis, keepdims=False)


def gather(own):
    lines = lax.axis_size("fs") // 4
    line = [swap(own, "fs", 4 * k) for k in range(1, lines)]
    line = jnp.stack([own] + line)
    return [line] + [swap(line, "fs", c) for c in (1, 2, 3)]


def specs():
    return (pl.BlockSpec(memory_space=space) for space in (pltpu.SMEM, pltpu.VMEM, pl.ANY))


def directions(stacks, gram, factor, me):
    lines, rows, width = stacks[0].shape
    rank = gram.shape[0]
    if rows % 8:
        whole = jnp.zeros((4 * lines, rows, width), f32)
        for c, stack in enumerate(stacks):
            for k in range(lines):
                whole = lax.dynamic_update_index_in_dim(whole, stack[k], me ^ (4 * k + c), 0)
        stacks, lines = [whole.reshape(1, rank, width)], 1

    def terms_of(a, count):
        for _ in range(count):
            top = a.astype(bf16)
            yield top
            a = a - top.astype(f32)

    def kernel(me_ref, gram_ref, factor_ref, *refs):
        pieces, (moved_ref, square_ref, ratio_ref) = refs[:-3], refs[-3:]
        for c, stack in enumerate(pieces):
            for k in range(lines):
                if rows % 8:
                    ratio_ref[...] = stack[k]
                else:
                    owner = me_ref[0] ^ (4 * k + c)
                    ratio_ref[pl.ds(pl.multiple_of(owner * rows, rows), rows), :] = stack[k]
        ratio = ratio_ref[...]
        high, middle, low = terms_of(ratio, 3)
        some = factor_ref[...]
        moved_ref[...] = jnp.dot(
            jnp.concatenate([some] * 3, axis=1),
            jnp.concatenate([high, middle, low]),
            preferred_element_type=f32,
        )
        gram_high, gram_low = terms_of(gram_ref[...], 2)
        applied = jnp.dot(
            jnp.concatenate([gram_high, gram_high, gram_low], axis=1),
            jnp.concatenate([high, middle, high]),
            preferred_element_type=f32,
        )
        by_column = jnp.sum(ratio * applied, axis=0, keepdims=True)
        square = jnp.sum(by_column, axis=1, keepdims=True)
        square_ref[...] = jnp.broadcast_to(square, square_ref.shape)

    smem, vmem, _ = specs()
    return pl.pallas_call(
        kernel,
        out_shape=(
            jax.ShapeDtypeStruct((factor.shape[0], width), f32),
            jax.ShapeDtypeStruct((8, 128), f32),
        ),
        in_specs=[smem] + [vmem] * (2 + len(stacks)),
        out_specs=(vmem, vmem),
        scratch_shapes=[pltpu.VMEM((rank, width), f32)],
        cost_estimate=pl.CostEstimate(
            flops=6 * rank * width * (rank + factor.shape[0]),
            bytes_accessed=8 * rank * width,
            transcendentals=0,
        ),
        name="directions",
    )(me.astype(jnp.int32).reshape(1), gram, factor, *stacks)


def finish(moved, square, others, master, count):
    def kernel(moved_ref, square_ref, others_ref, master_ref, step_ref, copy_ref):
        mean = (square_ref[0:1, 0:1] + others_ref[0:1, 0:1]) / count
        step = moved_ref[...] * lax.rsqrt(mean + mean_floor)
        step_ref[...] = step
        copy_ref[...] = (master_ref[...] - step_size * step).astype(bf16)

    _, vmem, _ = specs()
    return pl.pallas_call(
        kernel,
        out_shape=(
            jax.ShapeDtypeStruct(moved.shape, f32),
            jax.ShapeDtypeStruct(moved.shape, bf16),
        ),
        in_specs=[vmem] * 4,
        out_specs=(vmem, vmem),
        cost_estimate=pl.CostEstimate(
            flops=4 * moved.size, bytes_accessed=14 * moved.size, transcendentals=0
        ),
        name="finish",
    )(moved, square, others, master)


def spread(own):
    lines = lax.axis_size("fs") // 4
    blocks = {}
    for k in range(lines):
        if k % 2 and k > 1:
            block = swap(blocks[4 * k - 4], "fs", 4)
        else:
            block = swap(own, "fs", 4 * k) if k else own
        across = swap(block, "fs", 1)
        along = swap(block, "fs", 2)
        if k % 2:
            corner = swap(blocks[4 * k - 1], "fs", 4)
        elif k % 4:
            corner = swap(along, "fs", 1)
        else:
            corner = swap(across, "fs", 2)
        blocks |= {4 * k: block, 4 * k + 1: across, 4 * k + 2: along, 4 * k + 3: corner}
    return blocks


def place_copies(blocks, me):
    lines = len(blocks) // 4
    order = []
    for k in range(lines):
        order += [4 * k, 4 * k + 1, 4 * k + 2] + [4 * k - 1] * (k > 0)
    order.append(4 * lines - 1)
    rows, width = blocks[0].shape
    out = None
    for start in range(0, len(order), 4):
        group = order[start : start + 4]

        def kernel(me_ref, *refs, group=group):
            sources, out_ref, sems = refs[: len(group)], refs[-2], refs[-1]
            copies = []
            for i, mask in enumerate(group):
                target = pl.ds(pl.multiple_of((me_ref[0] ^ mask) * rows, rows), rows)
                copies.append(pltpu.make_async_copy(sources[i], out_ref.at[target, :], sems.at[i]))
                copies[-1].start()
            for copy in copies:
                copy.wait()

        smem, vmem, anywhere = specs()
        n = len(group)
        call = pl.pallas_call(
            kernel,
            out_shape=jax.ShapeDtypeStruct((len(order) * rows, width), bf16),
            in_specs=[smem] + [vmem] * n + [anywhere] * (out is not None),
            out_specs=pl.BlockSpec(memory_space=pltpu.HBM),
            scratch_shapes=[pltpu.SemaphoreType.DMA((n,))],
            input_output_aliases={} if out is None else {1 + n: 0},
            cost_estimate=pl.CostEstimate(
                flops=0, bytes_accessed=4 * n * rows * width, transcendentals=0
            ),
            name="place_copies",
        )
        out = call(
            me.astype(jnp.int32).reshape(1),
            *(blocks[mask] for mask in group),
            *([] if out is None else [out]),
        )
    return out


def order_factors(mine, other, me, core):
    lines, rows, columns = mine[0].shape
    count = 4 * lines

    def kernel(me_ref, core_ref, *refs):
        sources, (out_in, out_gate) = refs[:-2], refs[-2:]
        first = core_ref[0] == 0
        for c in range(4):
            for k in range(lines):
                owner = me_ref[0] ^ (4 * k + c)
                target = pl.ds(pl.multiple_of(owner * rows, rows), rows)
                a, b = sources[c][k], sources[4 + c][k]
                out_in[target, :] = jnp.where(first, a, b)
                out_gate[target, :] = jnp.where(first, b, a)

    smem, vmem = (pl.BlockSpec(memory_space=space) for space in (pltpu.SMEM, pltpu.VMEM))
    shape = jax.ShapeDtypeStruct((count * rows, columns), mine[0].dtype)
    return pl.pallas_call(
        kernel,
        out_shape=(shape, shape),
        in_specs=[smem, smem] + [vmem] * 8,
        out_specs=(vmem, vmem),
        cost_estimate=pl.CostEstimate(
            flops=0, bytes_accessed=8 * count * rows * columns, transcendentals=0
        ),
        name="order_factors",
    )(me.astype(jnp.int32).reshape(1), core.astype(jnp.int32).reshape(1), *mine, *other)


def local(
    saved_inputs,
    input_cot,
    gate_cot,
    input_master,
    gate_master,
    input_factor,
    gate_factor,
    input_first,
    input_second,
    gate_first,
    gate_second,
):
    fs, tp = lax.axis_size("fs"), lax.axis_size("tp")
    me, core = lax.axis_index("fs"), lax.axis_index("tp")
    lines = fs // 4
    here_x, here_y, here_z = me & 1, (me >> 1) & 1, me >> 2
    rank = input_factor.shape[1]
    width = input_cot.shape[1]
    half = width // 2
    count = fs * input_master.shape[0] * tp * width

    if tp == 2:
        mine = gather(jnp.where(core == 0, input_factor, gate_factor))
        other = [swap(stack, "tp", 1) for stack in mine]
        whole_in, whole_gate = order_factors(mine, other, me, core)
    else:
        zero = jnp.zeros_like(core)
        whole_in, whole_gate = order_factors(gather(input_factor), gather(gate_factor), me, zero)

    def chain(cot, master, own_factor, factor, first, second):
        projected = split(dot(saved_inputs, factor, plain), 2)
        term = sum(dot(piece, cot, contract) for piece in projected)
        term = term.reshape(lines, 2, 2, rank // fs, width)
        left, right = term[..., :half], term[..., half:]
        left = pick(left, here_x, 2) + swap(pick(left, 1 - here_x, 2), "fs", 1)
        right = pick(right, here_y, 1) + swap(pick(right, 1 - here_y, 1), "fs", 2)
        left = pick(left, here_y, 1) + swap(pick(left, 1 - here_y, 1), "fs", 2)
        right = pick(right, here_x, 1) + swap(pick(right, 1 - here_x, 1), "fs", 1)
        both = jnp.concatenate([left, right], axis=-1)
        low_rank = pick(both, here_z, 0)
        for k in range(1, lines):
            low_rank = low_rank + swap(pick(both, here_z ^ k, 0), "fs", 4 * k)
        first_new, second_new, ratio = moments(low_rank, first, second)
        stacks = gather(ratio)
        gram = dot(factor, factor, contract)
        moved, square = directions(stacks, gram, own_factor, me)
        if tp == 2:
            others = swap(square, "tp", 1)
        else:
            others = lax.psum(square, "tp") - square
        step, local_copy = finish(moved, square, others, master, count)
        copy = place_copies(spread(local_copy), me)
        return step, first_new, second_new, copy

    step_gate, first_gate, second_gate, copy_gate = chain(
        gate_cot, gate_master, gate_factor, whole_gate, gate_first, gate_second
    )
    step_in, first_in, second_in, copy_in = chain(
        input_cot, input_master, input_factor, whole_in, input_first, input_second
    )
    return (step_in, step_gate, first_in, second_in, first_gate, second_gate, copy_in, copy_gate)


def solution(mesh):
    rows, tokens = P("fs", "tp"), P("fs", None)

    return jax.shard_map(
        local,
        mesh=mesh,
        in_specs=(tokens, rows, rows, rows, rows, tokens, tokens, rows, rows, rows, rows),
        out_specs=(rows,) * 6 + (P(None, "tp"),) * 2,
        check_vma=False,
    )
```

```python
import jax
import jax.numpy as jnp
from jax import lax
from jax.experimental import pallas as pl
from jax.experimental.pallas import tpu as pltpu
from jax.sharding import PartitionSpec as P

first_decay = 0.9
second_decay = 0.9
ratio_floor = 1e-08
mean_floor = 1e-06
step_size = 0.05
bf16 = jnp.bfloat16
f32 = jnp.float32
contract = (((0,), (0,)), ((), ()))
plain = (((1,), (0,)), ((), ()))


def swap(a, axis, mask):
    size = lax.axis_size(axis)
    return lax.ppermute(a, axis, [(i, i ^ mask) for i in range(size)])


def split(a, terms):
    out = []
    for _ in range(terms):
        top = lax.reduce_precision(a, 8, 7)
        out.append(top.astype(bf16))
        a = a - top
    return out


def dot(a, b, dims):
    return lax.dot_general(a, b, dims, preferred_element_type=f32)


def moments(low_rank, first, second):
    first_new = first_decay * first + (1.0 - first_decay) * low_rank
    second_new = second_decay * second + (1.0 - second_decay) * low_rank * low_rank
    ratio = first_new / (jnp.sqrt(second_new) + ratio_floor)
    return (first_new, second_new, ratio)


def pick(a, index, axis):
    return lax.dynamic_index_in_dim(a, index, axis, keepdims=False)


def gather(own):
    lines = lax.axis_size("fs") // 4
    line = [swap(own, "fs", 4 * k) for k in range(1, lines)]
    line = jnp.stack([own] + line)
    return [line] + [swap(line, "fs", c) for c in (1, 2, 3)]


def gather_rows(own, me):
    lines = lax.axis_size("fs") // 4
    line = [own] + [swap(own, "fs", 4 * k) for k in range(1, lines)]
    bit = 1
    while bit < lines:
        crossed = (me >> 2) & bit > 0
        line = [jnp.where(crossed, line[k ^ bit], line[k]) for k in range(lines)]
        bit *= 2
    line = jnp.concatenate(line)
    return [line] + [swap(line, "fs", c) for c in (1, 2, 3)]


def specs():
    return (pl.BlockSpec(memory_space=space) for space in (pltpu.SMEM, pltpu.VMEM, pl.ANY))


def directions(stacks, gram, factor, me):
    lines, rows, width = stacks[0].shape
    rank = gram.shape[0]
    if rows % 8:
        whole = jnp.zeros((4 * lines, rows, width), f32)
        for c, stack in enumerate(stacks):
            for k in range(lines):
                whole = lax.dynamic_update_index_in_dim(whole, stack[k], me ^ (4 * k + c), 0)
        stacks, lines = [whole.reshape(1, rank, width)], 1

    def terms_of(a, count):
        for _ in range(count):
            top = a.astype(bf16)
            yield top
            a = a - top.astype(f32)

    def kernel(me_ref, gram_ref, factor_ref, *refs):
        pieces, (moved_ref, square_ref, ratio_ref) = refs[:-3], refs[-3:]
        for c, stack in enumerate(pieces):
            for k in range(lines):
                if rows % 8:
                    ratio_ref[...] = stack[k]
                else:
                    owner = me_ref[0] ^ (4 * k + c)
                    ratio_ref[pl.ds(pl.multiple_of(owner * rows, rows), rows), :] = stack[k]
        ratio = ratio_ref[...]
        high, middle, low = terms_of(ratio, 3)
        some = factor_ref[...]
        moved_ref[...] = jnp.dot(
            jnp.concatenate([some] * 3, axis=1),
            jnp.concatenate([high, middle, low]),
            preferred_element_type=f32,
        )
        gram_high, gram_low = terms_of(gram_ref[...], 2)
        applied = jnp.dot(
            jnp.concatenate([gram_high, gram_high, gram_low], axis=1),
            jnp.concatenate([high, middle, high]),
            preferred_element_type=f32,
        )
        by_column = jnp.sum(ratio * applied, axis=0, keepdims=True)
        square = jnp.sum(by_column, axis=1, keepdims=True)
        square_ref[...] = jnp.broadcast_to(square, square_ref.shape)

    smem, vmem, _ = specs()
    return pl.pallas_call(
        kernel,
        out_shape=(
            jax.ShapeDtypeStruct((factor.shape[0], width), f32),
            jax.ShapeDtypeStruct((8, 128), f32),
        ),
        in_specs=[smem] + [vmem] * (2 + len(stacks)),
        out_specs=(vmem, vmem),
        scratch_shapes=[pltpu.VMEM((rank, width), f32)],
        cost_estimate=pl.CostEstimate(
            flops=6 * rank * width * (rank + factor.shape[0]),
            bytes_accessed=8 * rank * width,
            transcendentals=0,
        ),
        name="directions",
    )(me.astype(jnp.int32).reshape(1), gram, factor, *stacks)


def finish(moved, square, others, master, count):
    def kernel(moved_ref, square_ref, others_ref, master_ref, step_ref, copy_ref):
        mean = (square_ref[0:1, 0:1] + others_ref[0:1, 0:1]) / count
        step = moved_ref[...] * lax.rsqrt(mean + mean_floor)
        step_ref[...] = step
        copy_ref[...] = (master_ref[...] - step_size * step).astype(bf16)

    _, vmem, _ = specs()
    return pl.pallas_call(
        kernel,
        out_shape=(jax.ShapeDtypeStruct(moved.shape, f32), jax.ShapeDtypeStruct(moved.shape, bf16)),
        in_specs=[vmem] * 4,
        out_specs=(vmem, vmem),
        cost_estimate=pl.CostEstimate(
            flops=4 * moved.size, bytes_accessed=14 * moved.size, transcendentals=0
        ),
        name="finish",
    )(moved, square, others, master)


def spread(own):
    lines = lax.axis_size("fs") // 4
    blocks = {}
    for k in range(lines):
        if k % 2 and k > 1:
            block = swap(blocks[4 * k - 4], "fs", 4)
        else:
            block = swap(own, "fs", 4 * k) if k else own
        across = swap(block, "fs", 1)
        along = swap(block, "fs", 2)
        if k % 2:
            corner = swap(blocks[4 * k - 1], "fs", 4)
        elif k % 4:
            corner = swap(along, "fs", 1)
        else:
            corner = swap(across, "fs", 2)
        blocks |= {4 * k: block, 4 * k + 1: across, 4 * k + 2: along, 4 * k + 3: corner}
    return blocks


def place_copies(gate, other, me):
    lines = len(gate) // 4
    everything = list(range(4 * lines))
    early = [0, 1, 2, 4]
    middle = [4 * k + c for k in range(1, lines - 2) for c in (0, 1, 2)]
    middle += [4 * k for k in range(max(lines - 2, 1), lines)]
    later = [3] + [4 * k + c for k in range(max(lines - 2, 0), lines - 1) for c in (1, 2)]
    groups = [(early, early), (middle, middle), (everything[:-1], later), (everything, everything)]
    rows, width = gate[0].shape
    shape = jax.ShapeDtypeStruct((4 * lines * rows, width), bf16)
    smem, vmem, anywhere = specs()
    outs, placed = (), (set(), set())
    for masks in groups:
        todo = []
        for i in (0, 1):
            todo += [(i, mask) for mask in masks[i] if mask < 4 * lines and mask not in placed[i]]
            placed[i].update(masks[i])
        n = len(todo)
        if not n:
            continue

        def kernel(me_ref, *refs, todo=todo, n=n):
            sources, targets, sems = refs[:n], refs[-3:-1], refs[-1]
            copies = []
            for at, (i, mask) in enumerate(todo):
                owner = me_ref[0] ^ mask
                rows_at = pl.ds(pl.multiple_of(owner * rows, rows), rows)
                target = targets[i].at[rows_at, :]
                copies.append(pltpu.make_async_copy(sources[at], target, sems.at[at]))
                copies[-1].start()
            for copy in copies:
                copy.wait()

        call = pl.pallas_call(
            kernel,
            out_shape=(shape, shape),
            in_specs=[smem] + [vmem] * n + [anywhere] * len(outs),
            out_specs=(pl.BlockSpec(memory_space=pltpu.HBM),) * 2,
            scratch_shapes=[pltpu.SemaphoreType.DMA((n,))],
            input_output_aliases={1 + n + i: i for i in range(len(outs))},
            cost_estimate=pl.CostEstimate(
                flops=0, bytes_accessed=4 * n * rows * width, transcendentals=0
            ),
            name="place_copies",
        )
        blocks = [(gate, other)[i][mask] for i, mask in todo]
        outs = call(me.astype(jnp.int32).reshape(1), *blocks, *outs)
    return outs


def local(
    saved_inputs,
    input_cot,
    gate_cot,
    input_master,
    gate_master,
    input_factor,
    gate_factor,
    input_first,
    input_second,
    gate_first,
    gate_second,
):
    fs, tp = lax.axis_size("fs"), lax.axis_size("tp")
    me, core = lax.axis_index("fs"), lax.axis_index("tp")
    lines = fs // 4
    here_x, here_y, here_z = me & 1, (me >> 1) & 1, me >> 2
    rank = input_factor.shape[1]
    width = input_cot.shape[1]
    half = width // 2
    count = fs * input_master.shape[0] * tp * width

    if tp == 2:
        mine = gather_rows(jnp.where(core == 0, input_factor, gate_factor), me)
        other = [swap(piece, "tp", 1) for piece in mine]
        factors_in = [jnp.where(core == 0, a, b) for a, b in zip(mine, other)]
        factors_gate = [jnp.where(core == 0, b, a) for a, b in zip(mine, other)]
    else:
        factors_in = gather_rows(input_factor, me)
        factors_gate = gather_rows(gate_factor, me)
    columns = saved_inputs.reshape(-1, lines, 4, input_factor.shape[0])
    columns = [pick(columns, (me & 3) ^ c, 2).reshape(saved_inputs.shape[0], -1) for c in range(4)]

    def chain(cot, master, own_factor, factors, first, second):
        projected = 0.0
        for c in range(4):
            projected += dot(columns[c], factors[c], plain)
        projected = split(projected, 2)
        term = sum(dot(piece, cot, contract) for piece in projected)
        term = term.reshape(lines, 2, 2, rank // fs, width)
        left, right = term[..., :half], term[..., half:]
        left = pick(left, here_x, 2) + swap(pick(left, 1 - here_x, 2), "fs", 1)
        right = pick(right, here_y, 1) + swap(pick(right, 1 - here_y, 1), "fs", 2)
        left = pick(left, here_y, 1) + swap(pick(left, 1 - here_y, 1), "fs", 2)
        right = pick(right, here_x, 1) + swap(pick(right, 1 - here_x, 1), "fs", 1)
        both = jnp.concatenate([left, right], axis=-1)
        low_rank = pick(both, here_z, 0)
        for k in range(1, lines):
            low_rank = low_rank + swap(pick(both, here_z ^ k, 0), "fs", 4 * k)
        first_new, second_new, ratio = moments(low_rank, first, second)
        stacks = gather(ratio)
        gram = sum(dot(piece, piece, contract) for piece in factors)
        moved, square = directions(stacks, gram, own_factor, me)
        if tp == 2:
            others = swap(square, "tp", 1)
        else:
            others = lax.psum(square, "tp") - square
        step, local_copy = finish(moved, square, others, master, count)
        blocks = spread(local_copy)
        return step, first_new, second_new, blocks

    step_gate, first_gate, second_gate, blocks_gate = chain(
        gate_cot, gate_master, gate_factor, factors_gate, gate_first, gate_second
    )
    step_in, first_in, second_in, blocks_in = chain(
        input_cot, input_master, input_factor, factors_in, input_first, input_second
    )
    copy_gate, copy_in = place_copies(blocks_gate, blocks_in, me)
    return (step_in, step_gate, first_in, second_in, first_gate, second_gate, copy_in, copy_gate)


def solution(mesh):
    rows, tokens = P("fs", "tp"), P("fs", None)

    return jax.shard_map(
        local,
        mesh=mesh,
        in_specs=(tokens, rows, rows, rows, rows, tokens, tokens, rows, rows, rows, rows),
        out_specs=(rows,) * 6 + (P(None, "tp"),) * 2,
        check_vma=False,
    )
```

```python
import jax
import jax.numpy as jnp
from jax import lax
from jax.experimental import pallas as pl
from jax.experimental.pallas import tpu as pltpu
from jax.sharding import PartitionSpec as P

first_decay = 0.9
second_decay = 0.9
ratio_floor = 1e-08
mean_floor = 1e-06
step_size = 0.05
bf16 = jnp.bfloat16
f32 = jnp.float32
contract = (((0,), (0,)), ((), ()))
plain = (((1,), (0,)), ((), ()))


def swap(a, axis, mask):
    size = lax.axis_size(axis)
    return lax.ppermute(a, axis, [(i, i ^ mask) for i in range(size)])


def split(a, terms):
    out = []
    for _ in range(terms):
        top = lax.reduce_precision(a, 8, 7)
        out.append(top.astype(bf16))
        a = a - top
    return out


def dot(a, b, dims):
    return lax.dot_general(a, b, dims, preferred_element_type=f32)


def moments(low_rank, first, second):
    first_new = first_decay * first + (1.0 - first_decay) * low_rank
    second_new = second_decay * second + (1.0 - second_decay) * low_rank * low_rank
    ratio = first_new / (jnp.sqrt(second_new) + ratio_floor)
    return (first_new, second_new, ratio)


def pick(a, index, axis):
    return lax.dynamic_index_in_dim(a, index, axis, keepdims=False)


def gather(own):
    lines = lax.axis_size("fs") // 4
    line = [swap(own, "fs", 4 * k) for k in range(1, lines)]
    line = jnp.stack([own] + line)
    return [line] + [swap(line, "fs", c) for c in (1, 2, 3)]


def gather_rows(own, me):
    lines = lax.axis_size("fs") // 4
    line = [own] + [swap(own, "fs", 4 * k) for k in range(1, lines)]
    bit = 1
    while bit < lines:
        crossed = (me >> 2) & bit > 0
        line = [jnp.where(crossed, line[k ^ bit], line[k]) for k in range(lines)]
        bit *= 2
    line = jnp.concatenate(line)
    return [line] + [swap(line, "fs", c) for c in (1, 2, 3)]


def specs():
    return (pl.BlockSpec(memory_space=space) for space in (pltpu.SMEM, pltpu.VMEM, pl.ANY))


def directions(stacks, gram, factor, me):
    lines, rows, width = stacks[0].shape
    rank = gram.shape[0]
    if rows % 8:
        whole = jnp.zeros((4 * lines, rows, width), f32)
        for c, stack in enumerate(stacks):
            for k in range(lines):
                whole = lax.dynamic_update_index_in_dim(whole, stack[k], me ^ (4 * k + c), 0)
        stacks, lines = [whole.reshape(1, rank, width)], 1

    def terms_of(a, count):
        for _ in range(count):
            top = a.astype(bf16)
            yield top
            a = a - top.astype(f32)

    def kernel(me_ref, gram_ref, factor_ref, *refs):
        pieces, (moved_ref, square_ref, ratio_ref) = refs[:-3], refs[-3:]
        for c, stack in enumerate(pieces):
            for k in range(lines):
                if rows % 8:
                    ratio_ref[...] = stack[k]
                else:
                    owner = me_ref[0] ^ (4 * k + c)
                    ratio_ref[pl.ds(pl.multiple_of(owner * rows, rows), rows), :] = stack[k]
        ratio = ratio_ref[...]
        high, middle, low = terms_of(ratio, 3)
        some = factor_ref[...]
        moved_ref[...] = jnp.dot(
            jnp.concatenate([some] * 3, axis=1),
            jnp.concatenate([high, middle, low]),
            preferred_element_type=f32,
        )
        gram_high, gram_low = terms_of(gram_ref[...], 2)
        applied = jnp.dot(
            jnp.concatenate([gram_high, gram_high, gram_low], axis=1),
            jnp.concatenate([high, middle, high]),
            preferred_element_type=f32,
        )
        by_column = jnp.sum(ratio * applied, axis=0, keepdims=True)
        square = jnp.sum(by_column, axis=1, keepdims=True)
        square_ref[...] = jnp.broadcast_to(square, square_ref.shape)

    smem, vmem, _ = specs()
    return pl.pallas_call(
        kernel,
        out_shape=(
            jax.ShapeDtypeStruct((factor.shape[0], width), f32),
            jax.ShapeDtypeStruct((8, 128), f32),
        ),
        in_specs=[smem] + [vmem] * (2 + len(stacks)),
        out_specs=(vmem, vmem),
        scratch_shapes=[pltpu.VMEM((rank, width), f32)],
        cost_estimate=pl.CostEstimate(
            flops=6 * rank * width * (rank + factor.shape[0]),
            bytes_accessed=8 * rank * width,
            transcendentals=0,
        ),
        compiler_params=pltpu.CompilerParams(vmem_limit_bytes=16 * 2**20),
        name="directions",
    )(me.astype(jnp.int32).reshape(1), gram, factor, *stacks)


def finish(moved, square, others, master, count):
    def kernel(moved_ref, square_ref, others_ref, master_ref, step_ref, copy_ref):
        mean = (square_ref[0:1, 0:1] + others_ref[0:1, 0:1]) / count
        step = moved_ref[...] * lax.rsqrt(mean + mean_floor)
        step_ref[...] = step
        copy_ref[...] = (master_ref[...] - step_size * step).astype(bf16)

    _, vmem, _ = specs()
    return pl.pallas_call(
        kernel,
        out_shape=(jax.ShapeDtypeStruct(moved.shape, f32), jax.ShapeDtypeStruct(moved.shape, bf16)),
        in_specs=[vmem] * 4,
        out_specs=(vmem, vmem),
        cost_estimate=pl.CostEstimate(
            flops=4 * moved.size, bytes_accessed=14 * moved.size, transcendentals=0
        ),
        compiler_params=pltpu.CompilerParams(vmem_limit_bytes=16 * 2**20),
        name="finish",
    )(moved, square, others, master)


def spread(own):
    lines = lax.axis_size("fs") // 4
    blocks = {}
    for k in range(lines):
        if k % 2 and k > 1:
            block = swap(blocks[4 * k - 4], "fs", 4)
        else:
            block = swap(own, "fs", 4 * k) if k else own
        across = swap(block, "fs", 1)
        along = swap(block, "fs", 2)
        if k % 2:
            corner = swap(blocks[4 * k - 1], "fs", 4)
        elif k % 4:
            corner = swap(along, "fs", 1)
        else:
            corner = swap(across, "fs", 2)
        blocks |= {4 * k: block, 4 * k + 1: across, 4 * k + 2: along, 4 * k + 3: corner}
    return blocks


def place_copies(gate, other, me):
    lines = len(gate) // 4
    everything = list(range(4 * lines))
    early = [0, 1, 2, 4]
    middle = [4 * k + c for k in range(1, lines - 2) for c in (0, 1, 2)]
    middle += [4 * k for k in range(max(lines - 2, 1), lines)]
    later = [3] + [4 * k + c for k in range(max(lines - 2, 0), lines - 1) for c in (1, 2, 3)]
    groups = [(early, early), (middle, middle), (everything[:-1], later), (everything, everything)]
    rows, width = gate[0].shape
    shape = jax.ShapeDtypeStruct((4 * lines * rows, width), bf16)
    smem, vmem, anywhere = specs()
    outs, placed = (), (set(), set())
    for masks in groups:
        todo = []
        for i in (0, 1):
            todo += [(i, mask) for mask in masks[i] if mask < 4 * lines and mask not in placed[i]]
            placed[i].update(masks[i])
        n = len(todo)
        if not n:
            continue

        def kernel(me_ref, *refs, todo=todo, n=n):
            sources, targets, sems = refs[:n], refs[-3:-1], refs[-1]
            copies = []
            for at, (i, mask) in enumerate(todo):
                owner = me_ref[0] ^ mask
                rows_at = pl.ds(pl.multiple_of(owner * rows, rows), rows)
                target = targets[i].at[rows_at, :]
                copies.append(pltpu.make_async_copy(sources[at], target, sems.at[at]))
                copies[-1].start()
            for copy in copies:
                copy.wait()

        call = pl.pallas_call(
            kernel,
            out_shape=(shape, shape),
            in_specs=[smem] + [vmem] * n + [anywhere] * len(outs),
            out_specs=(pl.BlockSpec(memory_space=pltpu.HBM),) * 2,
            scratch_shapes=[pltpu.SemaphoreType.DMA((n,))],
            input_output_aliases={1 + n + i: i for i in range(len(outs))},
            cost_estimate=pl.CostEstimate(
                flops=0, bytes_accessed=4 * n * rows * width, transcendentals=0
            ),
            compiler_params=pltpu.CompilerParams(vmem_limit_bytes=16 * 2**20),
        name="place_copies",
        )
        blocks = [(gate, other)[i][mask] for i, mask in todo]
        outs = call(me.astype(jnp.int32).reshape(1), *blocks, *outs)
    return outs


def local(
    saved_inputs,
    input_cot,
    gate_cot,
    input_master,
    gate_master,
    input_factor,
    gate_factor,
    input_first,
    input_second,
    gate_first,
    gate_second,
):
    fs, tp = lax.axis_size("fs"), lax.axis_size("tp")
    me, core = lax.axis_index("fs"), lax.axis_index("tp")
    lines = fs // 4
    here_x, here_y, here_z = me & 1, (me >> 1) & 1, me >> 2
    rank = input_factor.shape[1]
    width = input_cot.shape[1]
    half = width // 2
    count = fs * input_master.shape[0] * tp * width

    if tp == 2:
        mine = gather_rows(jnp.where(core == 0, input_factor, gate_factor), me)
        other = [swap(piece, "tp", 1) for piece in mine]
        factors_in = [jnp.where(core == 0, a, b) for a, b in zip(mine, other)]
        factors_gate = [jnp.where(core == 0, b, a) for a, b in zip(mine, other)]
    else:
        factors_in = gather_rows(input_factor, me)
        factors_gate = gather_rows(gate_factor, me)
    columns = saved_inputs.reshape(-1, lines, 4, input_factor.shape[0])
    columns = [pick(columns, (me & 3) ^ c, 2).reshape(saved_inputs.shape[0], -1) for c in range(4)]

    def chain(cot, master, own_factor, factors, first, second):
        projected = 0.0
        for c in range(4):
            projected += dot(columns[c], factors[c], plain)
        projected = split(projected, 2)
        term = sum(dot(piece, cot, contract) for piece in projected)
        term = term.reshape(lines, 2, 2, rank // fs, width)
        left, right = term[..., :half], term[..., half:]
        left = pick(left, here_x, 2) + swap(pick(left, 1 - here_x, 2), "fs", 1)
        right = pick(right, here_y, 1) + swap(pick(right, 1 - here_y, 1), "fs", 2)
        left = pick(left, here_y, 1) + swap(pick(left, 1 - here_y, 1), "fs", 2)
        right = pick(right, here_x, 1) + swap(pick(right, 1 - here_x, 1), "fs", 1)
        both = jnp.concatenate([left, right], axis=-1)
        low_rank = pick(both, here_z, 0)
        for k in range(1, lines):
            low_rank = low_rank + swap(pick(both, here_z ^ k, 0), "fs", 4 * k)
        first_new, second_new, ratio = moments(low_rank, first, second)
        stacks = gather(ratio)
        gram = sum(dot(piece, piece, contract) for piece in factors)
        moved, square = directions(stacks, gram, own_factor, me)
        if tp == 2:
            others = swap(square, "tp", 1)
        else:
            others = lax.psum(square, "tp") - square
        step, local_copy = finish(moved, square, others, master, count)
        blocks = spread(local_copy)
        return step, first_new, second_new, blocks

    step_gate, first_gate, second_gate, blocks_gate = chain(
        gate_cot, gate_master, gate_factor, factors_gate, gate_first, gate_second
    )
    step_in, first_in, second_in, blocks_in = chain(
        input_cot, input_master, input_factor, factors_in, input_first, input_second
    )
    copy_gate, copy_in = place_copies(blocks_gate, blocks_in, me)
    return (step_in, step_gate, first_in, second_in, first_gate, second_gate, copy_in, copy_gate)


def solution(mesh):
    rows, tokens = P("fs", "tp"), P("fs", None)

    return jax.shard_map(
        local,
        mesh=mesh,
        in_specs=(tokens, rows, rows, rows, rows, tokens, tokens, rows, rows, rows, rows),
        out_specs=(rows,) * 6 + (P(None, "tp"),) * 2,
        check_vma=False,
    )
```
